32 devices in a mesh: sp: 8 (over z, y), tp: 4 (over x, core).
Axes of the slice: x: 2, y: 2, z: 4, core: 2. Of those that a mesh axis runs over, the one named last changes fastest.
Arguments:
- glu_value: bfloat16 [4096, 2048], P('sp', 'tp'), may hold values from -640 to 640
- glu_gate: bfloat16 [4096, 2048], P('sp', 'tp'), may hold values from -9 to 9
- conv_kernel: float32 [31, 2048], P(None, 'tp'), may hold values from -1 to 1
- norm_gain: float32 [2048], P('tp'), may hold values from 0.1 to 1.9
- mix_weight: bfloat16 [2048, 2048], P('tp'), may hold values from -0.125 to 0.125
- residual: bfloat16 [4096, 2048], P(('sp', 'tp')), may hold values from -6 to 6
- resid_gain: float32 [2048], replicated, may hold values from 0.1 to 1.9
- expert_ids: int32 [4096, 2], P(('sp', 'tp')), may hold values from 0 to 7, all different within a row; in each aligned block of 128 rows (0 to 127, 128 to 255, ...) at most 64 rows name the same one
- route_weight: float32 [4096, 2], P(('sp', 'tp')), may hold values from 0.05 to 0.5
- w_gate: bfloat16 [8, 2048, 2048], P('sp', None, 'tp'), may hold values from -0.5 to 0.5
- w_up: bfloat16 [8, 2048, 2048], P('sp', None, 'tp'), may hold values from -0.5 to 0.5
- w_down: bfloat16 [8, 2048, 2048], P('sp', 'tp'), may hold values from -0.03125 to 0.03125
- out_gain: float32 [2048], replicated, may hold values from 0.1 to 1.9
Outputs:
- blended: bfloat16 [4096, 2048], P(('sp', 'tp'))
The draws below stay inside these ranges and needn't reach their ends.
Inputs may be any that keep to these rules, and one draw needn't show every extreme that they name: `expert_ids`: in each aligned block of 128 rows (the rows of one device) no expert is named by more than 64 rows, a bound that some block reaches.
All inputs are finite; a program needn't handle non-finite values.
Results may differ from the reference program's by a relative error of at most 0.015.
Values may be sent and summed in bfloat16 or wider, within the bound.
A program may use at most 128 MiB of HBM per device.

```python
import math
from functools import partial
import jax
import jax.numpy as jnp
import numpy as np
from jax import lax

D = 2048
DC = 2048
FFE = 2048
KERNEL = 31
TOPK = 2
TOKENS = 4096
BLOCK = 128
EXPERTS = 8
CAP = 64
N_SP = 8
N_TP = 4


def draw_glu_value(key, part):
    key_rough, key_base = jax.random.split(key, 2)
    ramp = 10.0 ** (jnp.arange(DC, dtype=jnp.float32) / DC)
    rough = jax.random.uniform(key_rough, (DC,), jnp.float32, 0.5, 1.5)
    base = jnp.clip(jax.random.normal(key_base, (TOKENS, DC), jnp.float32), -6.0, 6.0)
    return (0.5 * ramp * rough * base).astype(jnp.bfloat16)


def shard_levels(own_key, extent, cuts, least, high):
    level = 1.0
    for dim, shards_of in cuts:
        steps = jax.random.uniform(jax.random.fold_in(jax.random.fold_in(own_key, 6), dim), (shards_of,), jnp.float32, least / len(cuts), high / len(cuts))
        level = level * jnp.repeat(jnp.exp(steps), extent[dim] // shards_of).reshape((-1,) + (1,) * (len(extent) - 1 - dim))
    return level


def routed_block(rng, own, number, rows, number_of, top, bound, skew):
    order = jax.random.permutation(rng, number_of)
    crowded, usual = portions_of(number_of, rows * top, bound, skew, True), portions_of(number_of, rows * top, bound, skew, False)
    places = jnp.arange(number_of)

    def named(tallies, turn):
        used = int((tallies > 0).sum())
        fixed = max(1, used // 4)
        moved = fixed + (places - fixed + turn * (used - fixed)) % max(1, number_of - fixed)
        return jnp.zeros((number_of,), jnp.int32).at[order[jnp.where(places < fixed, places, moved)]].set(jnp.asarray(tallies, jnp.int32))

    tallies = jnp.where(number % 4 == 0, named(crowded, number // 4), named(usual, number - number // 4 - 1))
    mixed = jax.random.permutation(jax.random.fold_in(own, 3), number_of)
    giver, sink = mixed[0:number_of // 2 * 2:2], mixed[1:number_of // 2 * 2:2]
    margin = jnp.minimum(tallies[giver] - 1, bound - tallies[sink]) // 2
    margin = jnp.where((giver == order[0]) | (sink == order[0]) | (tallies[sink] == 0), 0, jnp.maximum(margin, 0))
    moved = jax.random.randint(jax.random.fold_in(own, 4), (number_of // 2,), 0, 1 << 20) % (margin + 1)
    tallies = tallies.at[giver].add(-moved).at[sink].add(moved)
    items = jnp.searchsorted(jnp.cumsum(tallies), jnp.arange(rows * top), side="right").astype(jnp.int32)
    grid = items.reshape(top, rows).T
    grid = grid[jax.random.permutation(jax.random.fold_in(own, 1), rows)]
    turn = jax.random.randint(jax.random.fold_in(own, 2), (rows, 1), 0, top)
    return jnp.take_along_axis(grid, (jnp.arange(top)[None, :] + turn) % top, axis=1)


def portions_of(number_of, total, reach, skew, full):
    loads = [(1 << 20) // math.isqrt(rank ** skew) + 1 for rank in range(1, number_of + 1)]
    largest = reach if full else min(reach, max(-(-total // number_of), total * loads[0] // sum(loads)))
    least = 1 if total - largest >= number_of - 1 else 0
    holding, spare = [largest] + [least] * (number_of - 1), total - largest - least * (number_of - 1)
    while spare > 0:
        candidates = [i for i in range(1, number_of) if holding[i] < largest] or [i for i in range(1, number_of) if holding[i] < reach]
        mass, budget = sum([loads[i] for i in candidates]), spare
        for i in candidates:
            addition = min(reach - holding[i], max(1, budget * loads[i] // mass), spare)
            holding[i] = holding[i] + addition
            spare = spare - addition
    return np.array(holding)


def noise(stream_key, dims, scale, limit, cuts=(), kind=jnp.bfloat16):
    factor_of = shard_levels(stream_key, dims, cuts, -0.22, 0.18) if cuts else 1.0
    values = jax.random.normal(stream_key, dims, jnp.float32) * scale * factor_of
    return jnp.minimum(jnp.maximum(values, -limit), limit).astype(kind)


def setup_inputs(seed: int = 0) -> dict:
    splits = jax.random.split(jax.random.key(seed), 14)
    glu_value = draw_glu_value(jax.random.fold_in(splits[13], 71), 0)
    glu_gate = noise(splits[1], (TOKENS, DC), 1.5, 9.0, ((0, 8), (1, 4)))
    conv_kernel = noise(splits[2], (KERNEL, DC), KERNEL ** -0.5, 1.0, ((1, 4),), jnp.float32)
    norm_gain = jnp.clip(1.0 + 0.18 * jax.random.normal(splits[3], (DC,), jnp.float32), 0.1, 1.9)
    mix_weight = noise(splits[4], (DC, D), DC ** -0.5, 0.125, ((0, 4),))
    residual = noise(splits[5], (TOKENS, D), 1.0, 6.0, ((0, 32),))
    resid_gain = jnp.clip(1.0 + 0.18 * jax.random.normal(splits[6], (D,), jnp.float32), 0.1, 1.9)
    expert_ids_keys = jax.random.split(jax.random.fold_in(splits[7], 1), TOKENS // BLOCK)
    expert_ids_turns = jax.random.permutation(jax.random.fold_in(splits[7], 3), TOKENS // BLOCK)
    expert_ids = jax.vmap(lambda own, number: routed_block(jax.random.fold_in(splits[7], 2), own, number, BLOCK, EXPERTS, TOPK, CAP, 2))(expert_ids_keys, expert_ids_turns).reshape((TOKENS, TOPK))
    route_weight = jnp.clip(jnp.exp(math.log(0.5) - 2.3025851 * jax.random.uniform(splits[8], (TOKENS, TOPK), jnp.float32) ** shard_levels(splits[8], (TOKENS, TOPK), ((0, 32),), -0.2, 0.2)), 0.05, 0.5)
    w_gate = noise(splits[9], (EXPERTS, D, FFE), (D // 16) ** -0.5, 0.5, ((0, 8), (2, 4)))
    w_up = noise(splits[10], (EXPERTS, D, FFE), (D // 16) ** -0.5, 0.5, ((0, 8), (2, 4)))
    w_down = noise(splits[11], (EXPERTS, FFE, D), (16 * FFE) ** -0.5, 0.03125, ((0, 8), (1, 4)))
    out_gain = jnp.clip(1.0 + 0.18 * jax.random.normal(splits[12], (D,), jnp.float32), 0.1, 1.9)
    return {"glu_value": glu_value, "glu_gate": glu_gate, "conv_kernel": conv_kernel, "norm_gain": norm_gain, "mix_weight": mix_weight, "residual": residual, "resid_gain": resid_gain, "expert_ids": expert_ids, "route_weight": route_weight, "w_gate": w_gate, "w_up": w_up, "w_down": w_down, "out_gain": out_gain}


EPSILON = 1e-05
LIMIT = 7.0
SLOPE = 1.702

def normalize(values, gain_vector):
    centre = lax.optimization_barrier(jnp.mean(values, axis=-1, keepdims=True))
    spread = lax.optimization_barrier(jnp.mean(jnp.square(values - centre), axis=-1, keepdims=True))
    return (values - centre) * lax.rsqrt(spread + EPSILON) * gain_vector

def slot_layout(route_ids, experts, capacity):
    row_count, top_count = route_ids.shape
    flat_ids = route_ids.reshape(row_count * top_count).astype(jnp.int32)
    onehot = (flat_ids[:, None] == jnp.arange(experts, dtype=jnp.int32)[None, :]).astype(jnp.int32)
    before = jnp.cumsum(onehot, axis=0) - onehot
    slot_rank = lax.optimization_barrier(jnp.sum(before * onehot, axis=1)).astype(jnp.int32)
    position = (flat_ids * capacity + slot_rank).astype(jnp.int32)
    owners = (jnp.arange(row_count * top_count, dtype=jnp.int32) // top_count).astype(jnp.int32)
    slot_table = jnp.full((experts * capacity,), row_count, jnp.int32).at[position].set(owners)
    return (slot_table, position.reshape(row_count, top_count))

def run_expert(operands):
    tokens, gate_matrix, up_matrix, down_matrix = operands
    tokens_wide = tokens.astype(jnp.float32)
    gate_pre = jnp.dot(tokens_wide, gate_matrix.astype(jnp.float32), preferred_element_type=jnp.float32)
    up_pre = jnp.dot(tokens_wide, up_matrix.astype(jnp.float32), preferred_element_type=jnp.float32)
    gated = jnp.minimum(gate_pre, LIMIT)
    upper = jnp.clip(up_pre, -LIMIT, LIMIT)
    activity = ((upper + 1.0) * gated * jax.nn.sigmoid(SLOPE * gated)).astype(jnp.bfloat16)
    quarter = FFE // N_TP
    pieces = activity.reshape(-1, N_TP, quarter).astype(jnp.float32)
    downs = down_matrix.reshape(N_TP, quarter, D).astype(jnp.float32)
    partials = jnp.einsum('rqf,qfd->qrd', pieces, downs).astype(jnp.bfloat16)
    partials = lax.optimization_barrier(partials)
    return lax.optimization_barrier(jnp.sum(partials.astype(jnp.float32), axis=0)).astype(jnp.bfloat16)

def reference(glu_value, glu_gate, conv_kernel, norm_gain, mix_weight, residual, resid_gain, expert_ids, route_weight, w_gate, w_up, w_down, out_gain):
    gated_in = (glu_value.astype(jnp.float32) * jax.nn.sigmoid(glu_gate.astype(jnp.float32))).astype(jnp.bfloat16)
    extended = jnp.pad(gated_in.astype(jnp.float32), ((KERNEL - 1, 0), (0, 0)))
    convolved = jnp.zeros((TOKENS, DC), jnp.float32)
    for offset in range(KERNEL):
        convolved = convolved + conv_kernel[offset] * extended[offset:offset + TOKENS]
    centre = lax.optimization_barrier(jnp.mean(convolved, axis=1, keepdims=True))
    spread = lax.optimization_barrier(jnp.mean(jnp.square(convolved), axis=1, keepdims=True)) - centre * centre
    normed = (convolved - centre) * lax.rsqrt(spread + EPSILON) * norm_gain
    mix_in = jax.nn.silu(normed).astype(jnp.bfloat16)
    mixed_rows = jnp.dot(mix_in, mix_weight, preferred_element_type=jnp.float32)
    hidden = normalize(residual.astype(jnp.float32) + mixed_rows, resid_gain).astype(jnp.bfloat16)
    block_count = N_SP * N_TP
    block_ids = expert_ids.reshape(block_count, BLOCK, TOPK)
    tables, positions = jax.vmap(partial(slot_layout, experts=EXPERTS, capacity=CAP))(block_ids)
    hidden_blocks = hidden.reshape(block_count, BLOCK, D)
    padded = jnp.concatenate([hidden_blocks, jnp.zeros((block_count, 1, D), jnp.bfloat16)], axis=1)
    slot_rows = jax.vmap(partial(jnp.take, axis=0))(padded, tables)
    expert_major = slot_rows.reshape(block_count, EXPERTS, CAP, D).transpose(1, 0, 2, 3)
    expert_major = expert_major.reshape(EXPERTS, block_count * CAP, D)
    outputs = lax.map(run_expert, (expert_major, w_gate, w_up, w_down))
    block_major = outputs.reshape(EXPERTS, block_count, CAP, D).transpose(1, 0, 2, 3)
    block_major = block_major.reshape(block_count, EXPERTS * CAP, D)
    picked = jax.vmap(partial(jnp.take, axis=0))(block_major, positions.reshape(block_count, BLOCK * TOPK))
    picked = picked.reshape(TOKENS, TOPK, D)
    routed_sum = jnp.einsum('tk,tkd->td', route_weight.astype(jnp.float32), picked.astype(jnp.float32))
    return normalize(hidden.astype(jnp.float32) + routed_sum, out_gain).astype(jnp.bfloat16)
```

```python
import functools

import jax
import jax.numpy as jnp
from jax import lax
from jax.experimental import pallas as pl
from jax.experimental.pallas import tpu as pltpu
from jax.sharding import PartitionSpec as P

DC = 2048


EPSILON = 1e-05
LIMIT = 7.0
SLOPE = 1.702


def shifted(block, axis, distance):
    devices = range(lax.axis_size(axis))
    route = [(i - distance, i) for i in devices if i - distance in devices]
    return lax.ppermute(block, axis, route)


def normalize(values, gain_vector):
    centre = jnp.mean(values, axis=-1, keepdims=True)
    spread = jnp.mean(jnp.square(values - centre), axis=-1, keepdims=True)
    return (values - centre) * lax.rsqrt(spread + EPSILON) * gain_vector


def swapped(block, stride):
    route = [(i, i ^ stride) for i in range(lax.axis_size("tp"))]
    return lax.ppermute(block, "tp", route)


def slot_layout(route_ids, experts, capacity):
    row_count, top_count = route_ids.shape
    flat_ids = route_ids.reshape(row_count * top_count)
    onehot = (flat_ids[:, None] == jnp.arange(experts, dtype=jnp.int32)[None, :]).astype(jnp.int32)
    before = jnp.cumsum(onehot, axis=0) - onehot
    slot_rank = jnp.sum(before * onehot, axis=1)
    position = flat_ids * capacity + slot_rank
    return position.reshape(row_count, top_count)


MESH = pl.DeviceIdType.MESH
GROUPS = 8
ARRIVAL = (0, 1, 4, 2, 5, 3, 6, 7)
RETURN = (4, 5, 6, 7, 2, 3, 1, 0)


def flipped(index, mask):
    result = index
    bit = 1
    while bit <= mask:
        if mask & bit:
            result = result + bit - 2 * bit * lax.rem(lax.div(index, bit), 2)
        bit *= 2
    return result


def experts_kernel(
    count,
    slots,
    gate_hbm,
    up_hbm,
    down_hbm,
    out,
    rows,
    outp,
    nrecv,
    frecv,
    act,
    gate,
    up,
    down,
    weight_sem,
    local_sem,
    disp_send,
    disp_recv,
    hop_send,
    hop_recv,
    ret_send,
    ret_recv,
):
    total = slots.shape[0]
    cap = total // count
    size = total // GROUPS
    per = count // GROUPS
    me = lax.axis_index("sp")
    place = lax.axis_index("tp")
    near = flipped(place, 1)
    far = flipped(place, 2)
    hidden, width = down.shape

    loads = [
        pltpu.make_async_copy(source, target, weight_sem.at[i])
        for i, (source, target) in enumerate(((gate_hbm, gate), (up_hbm, up), (down_hbm, down)))
    ]
    for load in loads:
        load.start()

    barrier = pltpu.get_barrier_semaphore()
    for k in range(1, count):
        pl.semaphore_signal(barrier, inc=1, device_id={"sp": flipped(me, k)}, device_id_type=MESH)
    for other in (near, far):
        pl.semaphore_signal(barrier, inc=1, device_id={"tp": other}, device_id_type=MESH)
    pl.semaphore_wait(barrier, count + 1)

    def spot(g, side):
        return pl.ds((2 * ARRIVAL.index(g) + side) * size, size)

    def spot_of(k):
        return pl.ds(2 * ARRIVAL.index(k // per) * size + (k % per) * cap, cap)

    def slots_of(index):
        return pl.ds(pl.multiple_of(index * cap, cap), cap)

    def dispatch(k):
        peer = flipped(me, k)
        return pltpu.make_async_remote_copy(
            src_ref=slots.at[slots_of(peer)],
            dst_ref=rows.at[0, spot_of(k)],
            send_sem=disp_send.at[k],
            recv_sem=disp_recv.at[k],
            device_id={"sp": peer},
            device_id_type=MESH,
        )

    def giveback(k):
        peer = flipped(me, k)
        return pltpu.make_async_remote_copy(
            src_ref=outp.at[0, spot_of(k)],
            dst_ref=out.at[slots_of(me)],
            send_sem=ret_send.at[k],
            recv_sem=ret_recv.at[k],
            device_id={"sp": peer},
            device_id_type=MESH,
        )

    def hop(kind, g, source, target, other):
        return pltpu.make_async_remote_copy(
            src_ref=source,
            dst_ref=target,
            send_sem=hop_send.at[kind, g],
            recv_sem=hop_recv.at[kind, g],
            device_id={"tp": other},
            device_id_type=MESH,
        )

    def rows_near(g):
        return hop(0, g, rows.at[0, spot(g, 0)], rows.at[0, spot(g, 1)], near)

    def rows_far(g):
        return hop(1, g, rows.at[0, spot(g, 0)], rows.at[1, spot(g, 0)], far)

    def rows_far_near(g):
        return hop(2, g, rows.at[1, spot(g, 0)], rows.at[1, spot(g, 1)], near)

    def part_near(side, g):
        return hop(
            3 + side, g, outp.at[side, spot(g, 1)], nrecv.at[side, pl.ds(g * size, size)], near
        )

    def part_far(g):
        return hop(5, g, outp.at[1, spot(g, 0)], frecv.at[pl.ds(g * size, size)], far)

    kept = pltpu.make_async_copy(slots.at[slots_of(me)], rows.at[0, spot_of(0)], local_sem)
    kept.start()
    for g in ARRIVAL:
        for k in range(g * per, (g + 1) * per):
            if k:
                dispatch(k).start()

    def forward(g):
        for k in range(g * per, (g + 1) * per):
            if k:
                dispatch(k).wait_recv()
            else:
                kept.wait()
        rows_far(g).start()
        rows_near(g).start()

    def forward_far(g):
        rows_far(g).wait_recv()
        rows_far_near(g).start()

    def compute(side, pair):
        both = ARRIVAL[2 * pair : 2 * pair + 2]
        for g in both:
            (rows_far_near(g) if side else rows_near(g)).wait_recv()
        if side == 0 and pair == 0:
            loads[0].wait()
            loads[1].wait()
        tile = pl.ds(4 * pair * size, 4 * size)
        step = min(256, hidden)

        @pl.loop(0, hidden // step)
        def _(j):
            columns = pl.ds(pl.multiple_of(j * step, step), step)
            tokens = rows[side, tile, :]
            gate_pre = jnp.dot(tokens, gate[:, columns], preferred_element_type=jnp.float32)
            up_pre = jnp.dot(tokens, up[:, columns], preferred_element_type=jnp.float32)
            gated = jnp.minimum(gate_pre, LIMIT)
            upper = jnp.clip(up_pre, -LIMIT, LIMIT)
            act[:, columns] = (
                (upper + 1.0) * gated * jax.nn.sigmoid(SLOPE * gated)
            ).astype(jnp.bfloat16)

        if side == 0 and pair == 0:
            loads[2].wait()
        wide = 512

        @pl.loop(0, width // wide)
        def _(j):
            columns = pl.ds(pl.multiple_of(j * wide, wide), wide)
            outp[side, tile, columns] = jnp.dot(
                act[...], down[:, columns], preferred_element_type=jnp.float32
            ).astype(jnp.bfloat16)

        for g in both:
            part_near(side, g).start()

    def chip_sum(g):
        part_near(1, g).wait_recv()
        mine = outp[1, spot(g, 0), :].astype(jnp.float32)
        other = nrecv[1, pl.ds(g * size, size), :].astype(jnp.float32)
        outp[1, spot(g, 0), :] = (mine + other).astype(jnp.bfloat16)
        part_far(g).start()

    home = pltpu.make_async_copy(outp.at[0, spot_of(0)], out.at[slots_of(me)], local_sem)

    def finish(g):
        part_near(0, g).wait_recv()
        mine = outp[0, spot(g, 0), :].astype(jnp.float32)
        other = nrecv[0, pl.ds(g * size, size), :].astype(jnp.float32)
        part_far(g).wait_recv()
        distant = frecv[pl.ds(g * size, size), :].astype(jnp.float32)
        outp[0, spot(g, 0), :] = (mine + other + distant).astype(jnp.bfloat16)
        for k in range(g * per, (g + 1) * per):
            if k:
                giveback(k).start()
            else:
                home.start()

    o = ARRIVAL
    forward(o[0])
    forward(o[1])
    forward_far(o[0])
    compute(0, 0)
    forward(o[2])
    forward(o[3])
    forward_far(o[1])
    compute(1, 0)
    compute(0, 1)
    forward(o[4])
    forward_far(o[2])
    forward_far(o[3])
    compute(1, 1)
    forward(o[5])
    compute(0, 2)
    forward_far(o[4])
    forward(o[6])
    forward(o[7])
    chip_sum(4)
    forward_far(o[5])
    compute(1, 2)
    compute(0, 3)
    chip_sum(5)
    forward_far(o[6])
    forward_far(o[7])
    compute(1, 3)
    for g in RETURN:
        if g not in (4, 5):
            chip_sum(g)
    for g in RETURN:
        finish(g)
    for k in range(1, count):
        dispatch(k).wait_send()
    for g in range(GROUPS):
        rows_near(g).wait_send()
        rows_far(g).wait_send()
        rows_far_near(g).wait_send()
        part_near(0, g).wait_send()
        part_near(1, g).wait_send()
        part_far(g).wait_send()
    home.wait()
    for k in range(1, count):
        giveback(k).wait()


def run_experts(count, slots, gate_matrix, up_matrix, down_matrix):
    total, width = slots.shape
    hidden = down_matrix.shape[0]
    size = total // GROUPS
    dtype = slots.dtype
    anywhere = pl.BlockSpec(memory_space=pl.ANY)
    return pl.pallas_call(
        functools.partial(experts_kernel, count),
        out_shape=jax.ShapeDtypeStruct(slots.shape, dtype),
        in_specs=[anywhere] * 4,
        out_specs=anywhere,
        scratch_shapes=[
            pltpu.VMEM((2, 2 * total, width), dtype),
            pltpu.VMEM((2, 2 * total, width), dtype),
            pltpu.VMEM((2, total, width), dtype),
            pltpu.VMEM((total, width), dtype),
            pltpu.VMEM((4 * size, hidden), dtype),
            pltpu.VMEM((width, hidden), dtype),
            pltpu.VMEM((width, hidden), dtype),
            pltpu.VMEM((hidden, width), dtype),
            pltpu.SemaphoreType.DMA((3,)),
            pltpu.SemaphoreType.DMA,
            pltpu.SemaphoreType.DMA((count,)),
            pltpu.SemaphoreType.DMA((count,)),
            pltpu.SemaphoreType.DMA((6, GROUPS)),
            pltpu.SemaphoreType.DMA((6, GROUPS)),
            pltpu.SemaphoreType.DMA((count,)),
            pltpu.SemaphoreType.DMA((count,)),
        ],
        compiler_params=pltpu.CompilerParams(
            collective_id=0, has_side_effects=True, vmem_limit_bytes=60 * 2**20
        ),
        cost_estimate=pl.CostEstimate(
            flops=24 * total * width * hidden,
            bytes_accessed=10 * total * width,
            transcendentals=4 * total * hidden,
        ),
        name="experts",
    )(slots, gate_matrix, up_matrix, down_matrix)


def shards(
    glu_value,
    glu_gate,
    conv_kernel,
    norm_gain,
    mix_weight,
    residual,
    resid_gain,
    expert_ids,
    route_weight,
    w_gate,
    w_up,
    w_down,
    out_gain,
):
    gate_local, up_local, down_local = w_gate[0], w_up[0], w_down[0]
    gated_in = (
        glu_value.astype(jnp.float32) * jax.nn.sigmoid(glu_gate.astype(jnp.float32))
    ).astype(jnp.bfloat16)
    reach_back = conv_kernel.shape[0] - 1
    length = gated_in.shape[0]
    before_rows = shifted(gated_in[length - reach_back :], "sp", 1)
    extended = jnp.concatenate([before_rows, gated_in], axis=0).astype(jnp.float32)
    convolved = jnp.zeros(gated_in.shape, jnp.float32)
    for offset in range(reach_back + 1):
        convolved = convolved + conv_kernel[offset] * extended[offset : offset + length]
    channel_sum, squares = lax.psum(
        (jnp.sum(convolved, axis=1), jnp.sum(convolved * convolved, axis=1)), "tp"
    )
    centre = channel_sum / DC
    spread = squares / DC - centre * centre
    normed = (convolved - centre[:, None]) * lax.rsqrt(spread[:, None] + EPSILON) * norm_gain
    mix_in = jax.nn.silu(normed).astype(jnp.bfloat16)
    tp_count = lax.axis_size("tp")
    place = lax.axis_index("tp")
    own_count = length // tp_count
    width = residual.shape[1]
    products = jnp.dot(mix_in, mix_weight, preferred_element_type=jnp.float32)
    products = products.astype(jnp.bfloat16).reshape(tp_count // 2, 2, own_count, width)
    near = place % 2
    far = place // 2
    kept = lax.dynamic_index_in_dim(products, near, 1, False)
    given = lax.dynamic_index_in_dim(products, 1 - near, 1, False)
    pair_sum = kept.astype(jnp.float32) + swapped(given, 1).astype(jnp.float32)
    pair_kept = lax.dynamic_index_in_dim(pair_sum, far, 0, False)
    pair_given = lax.dynamic_index_in_dim(pair_sum, 1 - far, 0, False).astype(jnp.bfloat16)
    mixed_rows = pair_kept + swapped(pair_given, 2).astype(jnp.float32)
    hidden = normalize(residual.astype(jnp.float32) + mixed_rows, resid_gain).astype(jnp.bfloat16)
    experts = lax.axis_size("sp")
    top_count = expert_ids.shape[1]
    capacity = 2 * own_count * top_count // experts
    positions = slot_layout(expert_ids, experts, capacity)
    slots = jnp.arange(experts * capacity, dtype=jnp.int32)
    chosen = (positions[:, :, None] == slots).astype(jnp.float32)
    pick = jnp.sum(chosen, axis=1).astype(jnp.bfloat16)
    weights = jnp.sum(chosen * route_weight[:, :, None], axis=1)
    weights_high = weights.astype(jnp.bfloat16)
    weights_low = (weights - weights_high.astype(jnp.float32)).astype(jnp.bfloat16)
    dispatched = lax.dot_general(
        pick, hidden, (((0,), (0,)), ((), ())), preferred_element_type=jnp.float32
    ).astype(jnp.bfloat16)
    returned = run_experts(experts, dispatched, gate_local, up_local, down_local)
    routed_sum = jnp.dot(weights_high, returned, preferred_element_type=jnp.float32) + jnp.dot(
        weights_low, returned, preferred_element_type=jnp.float32
    )
    return normalize(hidden.astype(jnp.float32) + routed_sum, out_gain).astype(jnp.bfloat16)


def solution(mesh):
    in_specs = (
        P("sp", "tp"),
        P("sp", "tp"),
        P(None, "tp"),
        P("tp"),
        P("tp", None),
        P(("sp", "tp"), None),
        P(),
        P(("sp", "tp"), None),
        P(("sp", "tp"), None),
        P("sp", None, "tp"),
        P("sp", None, "tp"),
        P("sp", "tp", None),
        P(),
    )
    out_specs = P(("sp", "tp"), None)

    return jax.shard_map(shards, mesh=mesh, in_specs=in_specs, out_specs=out_specs, check_vma=False)
```

```python
import functools

import jax
import jax.numpy as jnp
from jax import lax
from jax.experimental import pallas as pl
from jax.experimental.pallas import tpu as pltpu
from jax.sharding import PartitionSpec as P

EPSILON = 1e-05
LIMIT = 7.0
SLOPE = 1.702
HALO = 32
CHUNK = 64
PIECES = 4

MESH = pl.DeviceIdType.MESH
GROUPS = 8
ARRIVAL = (0, 1, 4, 2, 5, 3, 6, 7)
RETURN = (4, 5, 6, 7, 2, 3, 1, 0)


def flipped(index, mask):
    result = index
    bit = 1
    while bit <= mask:
        if mask & bit:
            result = result + bit - 2 * bit * lax.rem(lax.div(index, bit), 2)
        bit *= 2
    return result


def wide(values):
    return values.astype(jnp.float32)


def layer_kernel(
    count,
    places,
    value_hbm,
    glu_hbm,
    taps,
    norm_gain,
    mix_hbm,
    residual_hbm,
    resid_gain,
    ids,
    route,
    gate_hbm,
    up_hbm,
    down_hbm,
    out_gain,
    out,
    value,
    glu,
    mix,
    residual,
    gate,
    up,
    down,
    halo_out,
    halo_in,
    extended,
    convolved,
    stats,
    stats_in,
    mix_in,
    products,
    near_in,
    far_out,
    far_in,
    hidden,
    before,
    chosen,
    pick,
    weigh,
    high,
    low,
    slots,
    rows,
    outp,
    nrecv,
    frecv,
    act,
    returned,
    combined,
    load_sem,
    halo_send,
    halo_recv,
    stat_send,
    stat_recv,
    mixn_send,
    mixn_recv,
    mixf_send,
    mixf_recv,
    disp_send,
    disp_recv,
    hop_send,
    hop_recv,
    ret_send,
    ret_recv,
):
    me = lax.axis_index("sp")
    place = lax.axis_index("tp")
    near = flipped(place, 1)
    far = flipped(place, 2)
    across = flipped(place, 3)
    core = lax.rem(place, 2)
    side_x = lax.div(place, 2)

    length, channels = value.shape
    half = length // 2
    block = half // 2
    width = mix.shape[1]
    units = down.shape[0]
    total = slots.shape[0]
    cap = total // count
    size = total // GROUPS
    per = count // GROUPS
    piece = width // PIECES

    loads = [
        pltpu.make_async_copy(source, target, load_sem.at[i])
        for i, (source, target) in enumerate(
            (
                (value_hbm, value),
                (glu_hbm, glu),
                (mix_hbm, mix),
                (residual_hbm, residual),
                (gate_hbm, gate),
                (up_hbm, up),
                (down_hbm, down),
            )
        )
    ]
    for load in loads:
        load.start()

    following = lax.rem(me + 1, count)
    previous = lax.rem(me + count - 1, count)
    barrier = pltpu.get_barrier_semaphore()
    for k in range(1, count):
        pl.semaphore_signal(barrier, inc=1, device_id={"sp": flipped(me, k)}, device_id_type=MESH)
    for other in (near, far, across):
        pl.semaphore_signal(barrier, inc=1, device_id={"tp": other}, device_id_type=MESH)

    def gated(first, rows_at_once):
        span = pl.ds(first, rows_at_once)
        return (wide(value[span, :]) * jax.nn.sigmoid(wide(glu[span, :]))).astype(jnp.bfloat16)

    loads[0].wait()
    loads[1].wait()
    tail = gated(length - HALO, HALO)
    halo_out[...] = tail
    extended[pl.ds(length, HALO), :] = wide(tail)

    @pl.loop(0, length // CHUNK)
    def _(i):
        first = pl.multiple_of(i * CHUNK, CHUNK)
        extended[pl.ds(first + HALO, CHUNK), :] = wide(gated(first, CHUNK))

    pl.semaphore_wait(barrier, count + 2)
    halo = pltpu.make_async_remote_copy(
        src_ref=halo_out,
        dst_ref=halo_in,
        send_sem=halo_send,
        recv_sem=halo_recv,
        device_id={"sp": following},
        device_id_type=MESH,
    )

    @pl.when(me < count - 1)
    def _():
        halo.start()

    @pl.when(me > 0)
    def _():
        halo.wait_recv()
        extended[pl.ds(0, HALO), :] = wide(halo_in[...])

    @pl.when(me == 0)
    def _():
        extended[pl.ds(0, HALO), :] = jnp.zeros((HALO, channels), jnp.float32)

    lanes = lax.broadcasted_iota(jnp.int32, (8, 128), 1)
    origin = (half * (1 - side_x), half * side_x)

    def convolve(h):
        def step(i, carry):
            sums, squares = carry
            first = pl.multiple_of(origin[h] + i * CHUNK, CHUNK)
            row_sum = jnp.zeros((CHUNK, 128), jnp.float32)
            row_square = jnp.zeros((CHUNK, 128), jnp.float32)
            for c in range(channels // 128):
                columns = pl.ds(c * 128, 128)
                window = extended[pl.ds(first, CHUNK + HALO), columns]
                result = jnp.zeros((CHUNK, 128), jnp.float32)
                reach = taps.shape[0]
                lead = HALO - reach + 1
                for phase in range(8):
                    moved = window
                    if phase:
                        moved = pltpu.roll(window, CHUNK + HALO - phase, 0)
                    for k in range(reach):
                        if (k + lead) % 8 == phase:
                            start = (k + lead) // 8 * 8
                            result = result + taps[k : k + 1, columns] * moved[start : start + CHUNK]
                convolved[h, pl.ds(pl.multiple_of(i * CHUNK, CHUNK), CHUNK), columns] = result
                row_sum = row_sum + result
                row_square = row_square + result * result
            for r in range(CHUNK // 8):
                here = lanes == i * (CHUNK // 8) + r
                part = jnp.sum(row_sum[8 * r : 8 * r + 8], axis=1, keepdims=True)
                sums = jnp.where(here, part, sums)
                part = jnp.sum(row_square[8 * r : 8 * r + 8], axis=1, keepdims=True)
                squares = jnp.where(here, part, squares)
            return sums, squares

        zero = jnp.zeros((8, 128), jnp.float32)
        sums, squares = lax.fori_loop(0, half // CHUNK, step, (zero, zero))
        stats[h, 0] = sums
        stats[h, 1] = squares

    def stat_copy(h, j, other):
        theirs = 1 - h if j else h
        return pltpu.make_async_remote_copy(
            src_ref=stats.at[h],
            dst_ref=stats_in.at[theirs, j],
            send_sem=stat_send.at[h, j],
            recv_sem=stat_recv.at[theirs, j],
            device_id={"tp": other},
            device_id_type=MESH,
        )

    def stat_copies(h):
        return [stat_copy(h, j, other) for j, other in enumerate((near, far, across))]

    def normalized(h):
        stat_copies(h)[0].wait_recv()
        for copy in stat_copies(1 - h)[1:]:
            copy.wait_recv()
        both = stats[h] + stats_in[h, 0] + stats_in[h, 1] + stats_in[h, 2]
        centre = both[0] / (places * channels)
        scale = lax.rsqrt(both[1] / (places * channels) - centre * centre + EPSILON)

        @pl.loop(0, half // 16)
        def _(i):
            parts = []
            for r in range(2):
                here = lanes == 2 * i + r
                middle = jnp.sum(jnp.where(here, centre, 0.0), axis=1, keepdims=True)
                factor = jnp.sum(jnp.where(here, scale, 0.0), axis=1, keepdims=True)
                first = pl.multiple_of(i * 16 + r * 8, 8)
                normed = (convolved[h, pl.ds(first, 8), :] - middle) * factor * norm_gain[...]
                parts.append(jax.nn.silu(normed))
            span = pl.ds(pl.multiple_of(i * 16, 16), 16)
            mix_in[h, span, :] = jnp.concatenate(parts, axis=0).astype(jnp.bfloat16)

    kept_rows = pl.ds(pl.multiple_of(core * block, block), block)
    given_rows = pl.ds(pl.multiple_of((1 - core) * block, block), block)

    def mix_near(h, p):
        return pltpu.make_async_remote_copy(
            src_ref=products.at[h, p, given_rows],
            dst_ref=near_in.at[h, p],
            send_sem=mixn_send.at[h, p],
            recv_sem=mixn_recv.at[h, p],
            device_id={"tp": near},
            device_id_type=MESH,
        )

    def mix_far(p):
        return pltpu.make_async_remote_copy(
            src_ref=far_out.at[p],
            dst_ref=far_in.at[p],
            send_sem=mixf_send.at[p],
            recv_sem=mixf_recv.at[p],
            device_id={"tp": far},
            device_id_type=MESH,
        )

    def project(h):
        for p in range(PIECES):
            products[h, p] = jnp.dot(
                mix_in[h], mix[:, p * piece : (p + 1) * piece], preferred_element_type=jnp.float32
            ).astype(jnp.bfloat16)
            mix_near(h, p).start()

    convolve(0)
    for copy in stat_copies(0):
        copy.start()
    convolve(1)
    for copy in stat_copies(1):
        copy.start()

    experts = lax.broadcasted_iota(jnp.int32, (count, block), 0)
    named = [ids[j : j + 1, :] == experts for j in range(ids.shape[0])]
    hits = jnp.zeros((count, block), jnp.float32)
    shares = jnp.zeros((count, block), jnp.float32)
    for j, match in enumerate(named):
        hits = hits + jnp.where(match, 1.0, 0.0)
        shares = shares + jnp.where(match, route[j : j + 1, :], 0.0)
    earlier = lax.broadcasted_iota(jnp.int32, (block, block), 0)
    later = lax.broadcasted_iota(jnp.int32, (block, block), 1)
    triangle = jnp.where(earlier < later, 1.0, 0.0).astype(jnp.bfloat16)
    ranks = jnp.dot(hits.astype(jnp.bfloat16), triangle, preferred_element_type=jnp.float32)
    before[...] = jnp.where(hits > 0.0, ranks, -1.0)
    chosen[...] = shares
    rank = lax.broadcasted_iota(jnp.int32, (cap, block), 0).astype(jnp.float32)
    for k in range(count):
        expert = flipped(me, k)
        match = before[pl.ds(expert, 1), :] == rank
        pick[pl.ds(k * cap, cap), :] = jnp.where(match, 1.0, 0.0)
        weigh[pl.ds(k * cap, cap), :] = jnp.where(match, chosen[pl.ds(expert, 1), :], 0.0)
    turned = weigh[...].T
    upper_part = turned.astype(jnp.bfloat16)
    high[...] = upper_part
    low[...] = (turned - wide(upper_part)).astype(jnp.bfloat16)

    normalized(0)
    loads[2].wait()
    project(0)
    for p in range(PIECES):
        mix_near(0, p).wait_recv()
        far_out[p] = (wide(products[0, p, kept_rows, :]) + wide(near_in[0, p])).astype(jnp.bfloat16)
        mix_far(p).start()
    normalized(1)
    project(1)

    def normalize(values, gain):
        centred = values - jnp.mean(values, axis=1, keepdims=True)
        spread = jnp.mean(centred * centred, axis=1, keepdims=True)
        return centred * lax.rsqrt(spread + EPSILON) * gain

    loads[3].wait()
    for p in range(PIECES):
        mix_near(1, p).wait_recv()
    for p in range(PIECES):
        mix_far(p).wait_recv()

    @pl.loop(0, block // 16)
    def _(i):
        span = pl.ds(pl.multiple_of(i * 16, 16), 16)
        own = pl.ds(pl.multiple_of(core * block + i * 16, 16), 16)
        mixed = jnp.concatenate(
            [
                wide(products[1, p, own, :]) + wide(near_in[1, p, span, :]) + wide(far_in[p, span, :])
                for p in range(PIECES)
            ],
            axis=1,
        )
        hidden[span, :] = normalize(wide(residual[span, :]) + mixed, resid_gain[...]).astype(
            jnp.bfloat16
        )

    def spot(g, side):
        return pl.ds((2 * ARRIVAL.index(g) + side) * size, size)

    def spot_of(k):
        return pl.ds(2 * ARRIVAL.index(k // per) * size + (k % per) * cap, cap)

    def dispatch(k):
        return pltpu.make_async_remote_copy(
            src_ref=slots.at[pl.ds(k * cap, cap)],
            dst_ref=rows.at[0, spot_of(k)],
            send_sem=disp_send.at[k],
            recv_sem=disp_recv.at[k],
            device_id={"sp": flipped(me, k)},
            device_id_type=MESH,
        )

    def giveback(k):
        return pltpu.make_async_remote_copy(
            src_ref=outp.at[0, spot_of(k)],
            dst_ref=returned.at[pl.ds(k * cap, cap)],
            send_sem=ret_send.at[k],
            recv_sem=ret_recv.at[k],
            device_id={"sp": flipped(me, k)},
            device_id_type=MESH,
        )

    def hop(kind, g, source, target, other):
        return pltpu.make_async_remote_copy(
            src_ref=source,
            dst_ref=target,
            send_sem=hop_send.at[kind, g],
            recv_sem=hop_recv.at[kind, g],
            device_id={"tp": other},
            device_id_type=MESH,
        )

    def rows_near(g):
        return hop(0, g, rows.at[0, spot(g, 0)], rows.at[0, spot(g, 1)], near)

    def rows_far(g):
        return hop(1, g, rows.at[0, spot(g, 0)], rows.at[1, spot(g, 0)], far)

    def rows_far_near(g):
        return hop(2, g, rows.at[1, spot(g, 0)], rows.at[1, spot(g, 1)], near)

    def part_near(side, g):
        return hop(
            3 + side, g, outp.at[side, spot(g, 1)], nrecv.at[side, pl.ds(g * size, size)], near
        )

    def part_far(g):
        return hop(5, g, outp.at[1, spot(g, 0)], frecv.at[pl.ds(g * size, size)], far)

    def send_group(g):
        for k in range(g * per, (g + 1) * per):
            if k:
                dispatch(k).start()

    for index, g in enumerate(ARRIVAL):
        span = pl.ds(g * size, size)
        picked = jnp.dot(
            pick[span, :].astype(jnp.bfloat16), hidden[...], preferred_element_type=jnp.float32
        ).astype(jnp.bfloat16)
        slots[span, :] = picked
        if g == 0:
            rows[0, spot_of(0), :] = slots[pl.ds(0, cap), :]
        if index:
            send_group(ARRIVAL[index - 1])
    send_group(ARRIVAL[-1])

    def forward(g):
        for k in range(g * per, (g + 1) * per):
            if k:
                dispatch(k).wait_recv()
        rows_far(g).start()
        rows_near(g).start()

    def forward_far(g):
        rows_far(g).wait_recv()
        rows_far_near(g).start()

    def compute(side, pair):
        both = ARRIVAL[2 * pair : 2 * pair + 2]
        for g in both:
            (rows_far_near(g) if side else rows_near(g)).wait_recv()
        if side == 0 and pair == 0:
            loads[4].wait()
            loads[5].wait()
        tile = pl.ds(4 * pair * size, 4 * size)
        step = min(256, units)

        @pl.loop(0, units // step)
        def _(j):
            columns = pl.ds(pl.multiple_of(j * step, step), step)
            tokens = rows[side, tile, :]
            gate_pre = jnp.dot(tokens, gate[:, columns], preferred_element_type=jnp.float32)
            up_pre = jnp.dot(tokens, up[:, columns], preferred_element_type=jnp.float32)
            clipped = jnp.minimum(gate_pre, LIMIT)
            upper = jnp.clip(up_pre, -LIMIT, LIMIT)
            act[:, columns] = (
                (upper + 1.0) * clipped * jax.nn.sigmoid(SLOPE * clipped)
            ).astype(jnp.bfloat16)

        if side == 0 and pair == 0:
            loads[6].wait()

        @pl.loop(0, PIECES)
        def _(j):
            columns = pl.ds(pl.multiple_of(j * piece, piece), piece)
            outp[side, tile, columns] = jnp.dot(
                act[...], down[:, columns], preferred_element_type=jnp.float32
            ).astype(jnp.bfloat16)

        for g in both:
            part_near(side, g).start()

    def chip_sum(g):
        part_near(1, g).wait_recv()
        mine = wide(outp[1, spot(g, 0), :])
        other = wide(nrecv[1, pl.ds(g * size, size), :])
        outp[1, spot(g, 0), :] = (mine + other).astype(jnp.bfloat16)
        part_far(g).start()

    def finish(g):
        part_near(0, g).wait_recv()
        mine = wide(outp[0, spot(g, 0), :])
        other = wide(nrecv[0, pl.ds(g * size, size), :])
        part_far(g).wait_recv()
        distant = wide(frecv[pl.ds(g * size, size), :])
        outp[0, spot(g, 0), :] = (mine + other + distant).astype(jnp.bfloat16)
        for k in range(g * per, (g + 1) * per):
            if k:
                giveback(k).start()
            else:
                returned[pl.ds(0, cap), :] = outp[0, spot_of(0), :]

    o = ARRIVAL
    forward(o[0])
    forward(o[1])
    forward_far(o[0])
    compute(0, 0)
    forward(o[2])
    forward(o[3])
    forward_far(o[1])
    compute(1, 0)
    compute(0, 1)
    forward(o[4])
    forward_far(o[2])
    forward_far(o[3])
    compute(1, 1)
    forward(o[5])
    compute(0, 2)
    forward_far(o[4])
    forward(o[6])
    forward(o[7])
    chip_sum(4)
    forward_far(o[5])
    compute(1, 2)
    compute(0, 3)
    chip_sum(5)
    forward_far(o[6])
    forward_far(o[7])
    compute(1, 3)
    for g in RETURN:
        if g not in (4, 5):
            chip_sum(g)
    for g in RETURN:
        finish(g)

    for k in range(1, count):
        giveback(k).wait_recv()

    @pl.loop(0, PIECES)
    def _(j):
        columns = pl.ds(pl.multiple_of(j * piece, piece), piece)
        values = returned[:, columns]
        combined[:, columns] = jnp.dot(
            high[...], values, preferred_element_type=jnp.float32
        ) + jnp.dot(low[...], values, preferred_element_type=jnp.float32)

    @pl.loop(0, block // 16)
    def _(i):
        span = pl.ds(pl.multiple_of(i * 16, 16), 16)
        out[span, :] = normalize(
            wide(hidden[span, :]) + combined[span, :], out_gain[...]
        ).astype(jnp.bfloat16)

    @pl.when(me < count - 1)
    def _():
        halo.wait_send()

    for h in range(2):
        for copy in stat_copies(h):
            copy.wait_send()
        for p in range(PIECES):
            mix_near(h, p).wait_send()
    for p in range(PIECES):
        mix_far(p).wait_send()
    for k in range(1, count):
        dispatch(k).wait_send()
        giveback(k).wait_send()
    for g in range(GROUPS):
        rows_near(g).wait_send()
        rows_far(g).wait_send()
        rows_far_near(g).wait_send()
        part_near(0, g).wait_send()
        part_near(1, g).wait_send()
        part_far(g).wait_send()


def layer(
    glu_value,
    glu_gate,
    conv_kernel,
    norm_gain,
    mix_weight,
    residual,
    resid_gain,
    expert_ids,
    route_weight,
    w_gate,
    w_up,
    w_down,
    out_gain,
):
    count = lax.axis_size("sp")
    places = lax.axis_size("tp")
    length, channels = glu_value.shape
    block, width = residual.shape
    units = w_down.shape[1]
    top = expert_ids.shape[1]
    total = 2 * block * top
    size = total // GROUPS
    half = length // 2
    piece = width // PIECES
    low_type = glu_value.dtype
    anywhere = pl.BlockSpec(memory_space=pl.ANY)
    inside = pl.BlockSpec(memory_space=pltpu.VMEM)

    def vmem(*shape, dtype=low_type):
        return pltpu.VMEM(shape, dtype)

    def wide_vmem(*shape):
        return pltpu.VMEM(shape, jnp.float32)

    scratch = [
        vmem(length, channels),
        vmem(length, channels),
        vmem(channels, width),
        vmem(block, width),
        vmem(width, units),
        vmem(width, units),
        vmem(units, width),
        vmem(HALO, channels),
        vmem(HALO, channels),
        wide_vmem(length + HALO, channels),
        wide_vmem(2, half, channels),
        wide_vmem(2, 2, 8, 128),
        wide_vmem(2, places - 1, 2, 8, 128),
        vmem(2, half, channels),
        vmem(2, PIECES, half, piece),
        vmem(2, PIECES, block, piece),
        vmem(PIECES, block, piece),
        vmem(PIECES, block, piece),
        vmem(block, width),
        wide_vmem(count, block),
        wide_vmem(count, block),
        wide_vmem(total, block),
        wide_vmem(total, block),
        vmem(block, total),
        vmem(block, total),
        vmem(total, width),
        vmem(2, 2 * total, width),
        vmem(2, 2 * total, width),
        vmem(2, total, width),
        vmem(total, width),
        vmem(4 * size, units),
        vmem(total, width),
        wide_vmem(block, width),
        pltpu.SemaphoreType.DMA((7,)),
        pltpu.SemaphoreType.DMA,
        pltpu.SemaphoreType.DMA,
        pltpu.SemaphoreType.DMA((2, places - 1)),
        pltpu.SemaphoreType.DMA((2, places - 1)),
        pltpu.SemaphoreType.DMA((2, PIECES)),
        pltpu.SemaphoreType.DMA((2, PIECES)),
        pltpu.SemaphoreType.DMA((PIECES,)),
        pltpu.SemaphoreType.DMA((PIECES,)),
        pltpu.SemaphoreType.DMA((count,)),
        pltpu.SemaphoreType.DMA((count,)),
        pltpu.SemaphoreType.DMA((6, GROUPS)),
        pltpu.SemaphoreType.DMA((6, GROUPS)),
        pltpu.SemaphoreType.DMA((count,)),
        pltpu.SemaphoreType.DMA((count,)),
    ]
    return pl.pallas_call(
        functools.partial(layer_kernel, count, places),
        out_shape=jax.ShapeDtypeStruct((block, width), low_type),
        in_specs=[
            anywhere,
            anywhere,
            inside,
            inside,
            anywhere,
            anywhere,
            inside,
            inside,
            inside,
            anywhere,
            anywhere,
            anywhere,
            inside,
        ],
        out_specs=inside,
        scratch_shapes=scratch,
        compiler_params=pltpu.CompilerParams(
            collective_id=0, has_side_effects=True, vmem_limit_bytes=62 * 2**20
        ),
        cost_estimate=pl.CostEstimate(
            flops=24 * total * width * units,
            bytes_accessed=10 * total * width,
            transcendentals=4 * total * units,
        ),
        name="layer",
    )(
        glu_value,
        glu_gate,
        conv_kernel,
        norm_gain[None, :],
        mix_weight,
        residual,
        resid_gain[None, :],
        expert_ids.T,
        route_weight.T,
        w_gate[0],
        w_up[0],
        w_down[0],
        out_gain[None, :],
    )


def solution(mesh):
    in_specs = (
        P("sp", "tp"),
        P("sp", "tp"),
        P(None, "tp"),
        P("tp"),
        P("tp", None),
        P(("sp", "tp"), None),
        P(),
        P(("sp", "tp"), None),
        P(("sp", "tp"), None),
        P("sp", None, "tp"),
        P("sp", None, "tp"),
        P("sp", "tp", None),
        P(),
    )

    return jax.shard_map(
        layer,
        mesh=mesh,
        in_specs=in_specs,
        out_specs=P(("sp", "tp"), None),
        check_vma=False,
    )
```

```python
import functools

import jax
import jax.numpy as jnp
from jax import lax
from jax.experimental import pallas as pl
from jax.experimental.pallas import tpu as pltpu
from jax.sharding import PartitionSpec as P

EPSILON = 1e-05
LIMIT = 7.0
SLOPE = 1.702
HALO = 32
CHUNK = 64
PIECES = 4

MESH = pl.DeviceIdType.MESH
GROUPS = 8
ARRIVAL = (0, 1, 2, 4, 3, 5, 6, 7)


def flipped(index, mask):
    result = index
    bit = 1
    while bit <= mask:
        if mask & bit:
            result = result + bit - 2 * bit * lax.rem(lax.div(index, bit), 2)
        bit *= 2
    return result


def wide(values):
    return values.astype(jnp.float32)


def layer_kernel(
    count,
    places,
    value_hbm,
    glu_hbm,
    taps,
    norm_gain,
    mix_hbm,
    residual_hbm,
    resid_gain,
    ids,
    route,
    gate_hbm,
    up_hbm,
    down_hbm,
    out_gain,
    out,
    value,
    glu,
    mix,
    residual,
    gate,
    up,
    down,
    halo_out,
    halo_in,
    extended,
    convolved,
    stats,
    stats_in,
    mix_in,
    products,
    near_in,
    far_out,
    far_in,
    hidden,
    before,
    chosen,
    pick,
    weigh,
    high,
    low,
    slots,
    rows,
    outp,
    nrecv,
    frecv,
    act,
    returned,
    combined,
    load_sem,
    halo_send,
    halo_recv,
    stat_send,
    stat_recv,
    mixn_send,
    mixn_recv,
    mixf_send,
    mixf_recv,
    disp_send,
    disp_recv,
    hop_send,
    hop_recv,
    ret_send,
    ret_recv,
):
    me = lax.axis_index("sp")
    place = lax.axis_index("tp")
    near = flipped(place, 1)
    far = flipped(place, 2)
    across = flipped(place, 3)
    core = lax.rem(place, 2)
    side_x = lax.div(place, 2)

    length, channels = value.shape
    half = length // 2
    block = half // 2
    width = mix.shape[1]
    units = down.shape[0]
    total = slots.shape[0]
    cap = total // count
    size = total // GROUPS
    per = count // GROUPS
    piece = width // PIECES

    loads = [
        pltpu.make_async_copy(source, target, load_sem.at[i])
        for i, (source, target) in enumerate(
            (
                (value_hbm, value),
                (glu_hbm, glu),
                (mix_hbm, mix),
                (residual_hbm, residual),
                (gate_hbm, gate),
                (up_hbm, up),
                (down_hbm, down),
            )
        )
    ]
    for load in loads[:2]:
        load.start()

    following = lax.rem(me + 1, count)
    previous = lax.rem(me + count - 1, count)
    barrier = pltpu.get_barrier_semaphore()
    for k in range(1, count):
        pl.semaphore_signal(barrier, inc=1, device_id={"sp": flipped(me, k)}, device_id_type=MESH)
    for other in (near, far, across):
        pl.semaphore_signal(barrier, inc=1, device_id={"tp": other}, device_id_type=MESH)

    def gated(first, rows_at_once):
        span = pl.ds(first, rows_at_once)
        return (wide(value[span, :]) * jax.nn.sigmoid(wide(glu[span, :]))).astype(jnp.bfloat16)

    loads[0].wait()
    loads[1].wait()
    for load in loads[2:]:
        load.start()
    tail = gated(length - HALO, HALO)
    halo_out[...] = tail
    extended[pl.ds(length, HALO), :] = wide(tail)

    @pl.loop(0, length // CHUNK)
    def _(i):
        first = pl.multiple_of(i * CHUNK, CHUNK)
        extended[pl.ds(first + HALO, CHUNK), :] = wide(gated(first, CHUNK))

    pl.semaphore_wait(barrier, count + 2)
    halo = pltpu.make_async_remote_copy(
        src_ref=halo_out,
        dst_ref=halo_in,
        send_sem=halo_send,
        recv_sem=halo_recv,
        device_id={"sp": following},
        device_id_type=MESH,
    )

    @pl.when(me < count - 1)
    def _():
        halo.start()

    lanes = lax.broadcasted_iota(jnp.int32, (8, 128), 1)
    upper_first = (1, 0)
    turn = (1 - side_x, side_x)

    def convolve(h):
        def step(i, carry):
            sums, squares = carry
            first = pl.multiple_of(h * half + i * CHUNK, CHUNK)
            row_sum = jnp.zeros((CHUNK, 128), jnp.float32)
            row_square = jnp.zeros((CHUNK, 128), jnp.float32)
            for c in range(channels // 128):
                columns = pl.ds(c * 128, 128)
                window = extended[pl.ds(first, CHUNK + HALO), columns]
                result = jnp.zeros((CHUNK, 128), jnp.float32)
                reach = taps.shape[0]
                lead = HALO - reach + 1
                for phase in range(8):
                    moved = window
                    if phase:
                        moved = pltpu.roll(window, CHUNK + HALO - phase, 0)
                    for k in range(reach):
                        if (k + lead) % 8 == phase:
                            start = (k + lead) // 8 * 8
                            result = result + taps[k : k + 1, columns] * moved[start : start + CHUNK]
                convolved[h, pl.ds(pl.multiple_of(i * CHUNK, CHUNK), CHUNK), columns] = result
                row_sum = row_sum + result
                row_square = row_square + result * result
            for r in range(CHUNK // 8):
                here = lanes == i * (CHUNK // 8) + r
                part = jnp.sum(row_sum[8 * r : 8 * r + 8], axis=1, keepdims=True)
                sums = jnp.where(here, part, sums)
                part = jnp.sum(row_square[8 * r : 8 * r + 8], axis=1, keepdims=True)
                squares = jnp.where(here, part, squares)
            return sums, squares

        zero = jnp.zeros((8, 128), jnp.float32)
        sums, squares = lax.fori_loop(0, half // CHUNK, step, (zero, zero))
        stats[h, 0] = sums
        stats[h, 1] = squares

    def stat_copy(h, j, other):
        return pltpu.make_async_remote_copy(
            src_ref=stats.at[h],
            dst_ref=stats_in.at[h, j],
            send_sem=stat_send.at[h, j],
            recv_sem=stat_recv.at[h, j],
            device_id={"tp": other},
            device_id_type=MESH,
        )

    def stat_copies(h):
        return [stat_copy(h, j, other) for j, other in enumerate((near, far, across))]

    def normalized(order):
        h = turn[order]
        for copy in stat_copies(h):
            copy.wait_recv()
        both = stats[h] + stats_in[h, 0] + stats_in[h, 1] + stats_in[h, 2]
        centre = both[0] / (places * channels)
        scale = lax.rsqrt(both[1] / (places * channels) - centre * centre + EPSILON)

        @pl.loop(0, half // 16)
        def _(i):
            parts = []
            for r in range(2):
                here = lanes == 2 * i + r
                middle = jnp.sum(jnp.where(here, centre, 0.0), axis=1, keepdims=True)
                factor = jnp.sum(jnp.where(here, scale, 0.0), axis=1, keepdims=True)
                first = pl.multiple_of(i * 16 + r * 8, 8)
                normed = (convolved[h, pl.ds(first, 8), :] - middle) * factor * norm_gain[...]
                parts.append(jax.nn.silu(normed))
            span = pl.ds(pl.multiple_of(i * 16, 16), 16)
            mix_in[order, span, :] = jnp.concatenate(parts, axis=0).astype(jnp.bfloat16)

    kept_rows = pl.ds(pl.multiple_of(core * block, block), block)
    given_rows = pl.ds(pl.multiple_of((1 - core) * block, block), block)

    def mix_near(h, p):
        return pltpu.make_async_remote_copy(
            src_ref=products.at[h, p, given_rows],
            dst_ref=near_in.at[h, p],
            send_sem=mixn_send.at[h, p],
            recv_sem=mixn_recv.at[h, p],
            device_id={"tp": near},
            device_id_type=MESH,
        )

    def mix_far(p):
        return pltpu.make_async_remote_copy(
            src_ref=far_out.at[p],
            dst_ref=far_in.at[p],
            send_sem=mixf_send.at[p],
            recv_sem=mixf_recv.at[p],
            device_id={"tp": far},
            device_id_type=MESH,
        )

    def project(h):
        for p in range(PIECES):
            products[h, p] = jnp.dot(
                mix_in[h], mix[:, p * piece : (p + 1) * piece], preferred_element_type=jnp.float32
            ).astype(jnp.bfloat16)
            mix_near(h, p).start()

    for h in upper_first:
        if h == 0:
            @pl.when(me > 0)
            def _():
                halo.wait_recv()
                extended[pl.ds(0, HALO), :] = wide(halo_in[...])

            @pl.when(me == 0)
            def _():
                extended[pl.ds(0, HALO), :] = jnp.zeros((HALO, channels), jnp.float32)
        convolve(h)
        for copy in stat_copies(h):
            copy.start()

    experts = lax.broadcasted_iota(jnp.int32, (count, block), 0)
    named = [ids[j : j + 1, :] == experts for j in range(ids.shape[0])]
    hits = jnp.zeros((count, block), jnp.float32)
    shares = jnp.zeros((count, block), jnp.float32)
    for j, match in enumerate(named):
        hits = hits + jnp.where(match, 1.0, 0.0)
        shares = shares + jnp.where(match, route[j : j + 1, :], 0.0)
    earlier = lax.broadcasted_iota(jnp.int32, (block, block), 0)
    later = lax.broadcasted_iota(jnp.int32, (block, block), 1)
    triangle = jnp.where(earlier < later, 1.0, 0.0).astype(jnp.bfloat16)
    ranks = jnp.dot(hits.astype(jnp.bfloat16), triangle, preferred_element_type=jnp.float32)
    before[...] = jnp.where(hits > 0.0, ranks, -1.0)
    chosen[...] = shares
    rank = lax.broadcasted_iota(jnp.int32, (cap, block), 0).astype(jnp.float32)
    for k in range(count):
        expert = flipped(me, k)
        match = before[pl.ds(expert, 1), :] == rank
        pick[pl.ds(k * cap, cap), :] = jnp.where(match, 1.0, 0.0)
        weigh[pl.ds(k * cap, cap), :] = jnp.where(match, chosen[pl.ds(expert, 1), :], 0.0)
    turned = weigh[...].T
    upper_part = turned.astype(jnp.bfloat16)
    high[...] = upper_part
    low[...] = (turned - wide(upper_part)).astype(jnp.bfloat16)

    normalized(0)
    loads[2].wait()
    project(0)
    for p in range(PIECES):
        mix_near(0, p).wait_recv()
        far_out[p] = (wide(products[0, p, kept_rows, :]) + wide(near_in[0, p])).astype(jnp.bfloat16)
        mix_far(p).start()
    normalized(1)
    project(1)

    def normalize(values, gain):
        centred = values - jnp.mean(values, axis=1, keepdims=True)
        spread = jnp.mean(centred * centred, axis=1, keepdims=True)
        return centred * lax.rsqrt(spread + EPSILON) * gain

    loads[3].wait()
    for p in range(PIECES):
        mix_near(1, p).wait_recv()
        columns = pl.ds(p * piece, piece)
        combined[:, columns] = (
            wide(residual[:, columns]) + wide(products[1, p, kept_rows, :]) + wide(near_in[1, p])
        )
    for p in range(PIECES):
        mix_far(p).wait_recv()

    @pl.loop(0, block // 32)
    def _(i):
        span = pl.ds(pl.multiple_of(i * 32, 32), 32)
        distant = jnp.concatenate([wide(far_in[p, span, :]) for p in range(PIECES)], axis=1)
        hidden[span, :] = normalize(combined[span, :] + distant, resid_gain[...]).astype(
            jnp.bfloat16
        )

    def spot(g, side):
        return pl.ds((2 * ARRIVAL.index(g) + side) * size, size)

    def spot_of(k):
        return pl.ds(2 * ARRIVAL.index(k // per) * size + (k % per) * cap, cap)

    def dispatch(k):
        return pltpu.make_async_remote_copy(
            src_ref=slots.at[pl.ds(k * cap, cap)],
            dst_ref=rows.at[0, spot_of(k)],
            send_sem=disp_send.at[k],
            recv_sem=disp_recv.at[k],
            device_id={"sp": flipped(me, k)},
            device_id_type=MESH,
        )

    def giveback(k):
        return pltpu.make_async_remote_copy(
            src_ref=outp.at[0, spot_of(k)],
            dst_ref=returned.at[pl.ds(k * cap, cap)],
            send_sem=ret_send.at[k],
            recv_sem=ret_recv.at[k],
            device_id={"sp": flipped(me, k)},
            device_id_type=MESH,
        )

    def hop(kind, g, source, target, other):
        return pltpu.make_async_remote_copy(
            src_ref=source,
            dst_ref=target,
            send_sem=hop_send.at[kind, g],
            recv_sem=hop_recv.at[kind, g],
            device_id={"tp": other},
            device_id_type=MESH,
        )

    def rows_near(g):
        return hop(0, g, rows.at[0, spot(g, 0)], rows.at[0, spot(g, 1)], near)

    def rows_far(g):
        return hop(1, g, rows.at[0, spot(g, 0)], rows.at[1, spot(g, 0)], far)

    def rows_far_near(g):
        return hop(2, g, rows.at[1, spot(g, 0)], rows.at[1, spot(g, 1)], near)

    def part_near(side, g):
        return hop(
            3 + side, g, outp.at[side, spot(g, 1)], nrecv.at[side, pl.ds(g * size, size)], near
        )

    def part_far(g):
        return hop(5, g, outp.at[1, spot(g, 0)], frecv.at[pl.ds(g * size, size)], far)

    def forward(g):
        for k in range(g * per, (g + 1) * per):
            if k:
                dispatch(k).wait_recv()
        rows_far(g).start()
        rows_near(g).start()

    def send_group(g):
        for k in range(g * per, (g + 1) * per):
            if k:
                dispatch(k).start()
        if g == 0 and per == 1:
            forward(g)

    for index, g in enumerate(ARRIVAL):
        span = pl.ds(g * size, size)
        picked = jnp.dot(
            pick[span, :].astype(jnp.bfloat16), hidden[...], preferred_element_type=jnp.float32
        ).astype(jnp.bfloat16)
        slots[span, :] = picked
        if g == 0:
            rows[0, spot_of(0), :] = slots[pl.ds(0, cap), :]
        if index:
            send_group(ARRIVAL[index - 1])
    send_group(ARRIVAL[-1])
    if per > 1:
        forward(0)

    def forward_far(g):
        rows_far(g).wait_recv()
        rows_far_near(g).start()

    def compute(side, *both):
        for g in both:
            (rows_far_near(g) if side else rows_near(g)).wait_recv()
        if side == 0 and 0 in both:
            loads[4].wait()
            loads[5].wait()
        count_rows = 2 * size * len(both)
        tile = pl.ds(2 * ARRIVAL.index(both[0]) * size, count_rows)
        step = min(256, units)

        @pl.loop(0, units // step)
        def _(j):
            columns = pl.ds(pl.multiple_of(j * step, step), step)
            tokens = rows[side, tile, :]
            gate_pre = jnp.dot(tokens, gate[:, columns], preferred_element_type=jnp.float32)
            up_pre = jnp.dot(tokens, up[:, columns], preferred_element_type=jnp.float32)
            clipped = jnp.minimum(gate_pre, LIMIT)
            upper = jnp.clip(up_pre, -LIMIT, LIMIT)
            act[:count_rows, columns] = (
                (upper + 1.0) * clipped * jax.nn.sigmoid(SLOPE * clipped)
            ).astype(jnp.bfloat16)

        if side == 0 and 0 in both:
            loads[6].wait()

        @pl.loop(0, PIECES)
        def _(j):
            columns = pl.ds(pl.multiple_of(j * piece, piece), piece)
            outp[side, tile, columns] = jnp.dot(
                act[:count_rows, :], down[:, columns], preferred_element_type=jnp.float32
            ).astype(jnp.bfloat16)

        for g in both:
            part_near(side, g).start()

    def chip_sum(g):
        part_near(1, g).wait_recv()
        mine = wide(outp[1, spot(g, 0), :])
        other = wide(nrecv[1, pl.ds(g * size, size), :])
        outp[1, spot(g, 0), :] = (mine + other).astype(jnp.bfloat16)
        part_far(g).start()

    def finish(g):
        part_near(0, g).wait_recv()
        mine = wide(outp[0, spot(g, 0), :])
        other = wide(nrecv[0, pl.ds(g * size, size), :])
        part_far(g).wait_recv()
        distant = wide(frecv[pl.ds(g * size, size), :])
        outp[0, spot(g, 0), :] = (mine + other + distant).astype(jnp.bfloat16)
        for k in range(g * per, (g + 1) * per):
            if k:
                giveback(k).start()
            else:
                returned[pl.ds(0, cap), :] = outp[0, spot_of(0), :]

    def combine(pair):
        for k in range(2 * pair * per, 2 * (pair + 1) * per):
            if k:
                giveback(k).wait_recv()
        inner = slice(2 * pair * size, 2 * (pair + 1) * size)
        for p in range(PIECES):
            columns = slice(p * piece, (p + 1) * piece)
            values = returned[inner, columns]
            combined[:, columns] += jnp.dot(
                high[:, inner], values, preferred_element_type=jnp.float32
            ) + jnp.dot(low[:, inner], values, preferred_element_type=jnp.float32)

    forward(1)
    forward_far(0)
    compute(0, 0, 1)
    forward(2)
    forward(4)
    forward_far(1)
    compute(1, 0, 1)
    compute(0, 2, 4)
    forward(3)
    forward_far(2)
    forward_far(4)
    compute(1, 2, 4)
    forward(5)
    chip_sum(4)
    compute(0, 3, 5)
    forward_far(3)
    forward(6)
    forward_far(5)
    compute(1, 3, 5)
    forward(7)
    chip_sum(5)
    chip_sum(2)
    compute(0, 6, 7)
    finish(4)
    forward_far(6)
    compute(1, 6)
    finish(5)
    chip_sum(6)
    forward_far(7)
    compute(1, 7)
    chip_sum(7)
    chip_sum(3)
    chip_sum(1)
    chip_sum(0)
    combined[...] = wide(hidden[...])
    finish(2)
    finish(6)
    finish(7)
    finish(3)
    combine(2)
    finish(1)
    combine(3)
    finish(0)
    combine(1)
    combine(0)

    @pl.loop(0, block // 32)
    def _(i):
        span = pl.ds(pl.multiple_of(i * 32, 32), 32)
        out[span, :] = normalize(combined[span, :], out_gain[...]).astype(jnp.bfloat16)

    @pl.when(me < count - 1)
    def _():
        halo.wait_send()

    for h in range(2):
        for copy in stat_copies(h):
            copy.wait_send()
        for p in range(PIECES):
            mix_near(h, p).wait_send()
    for p in range(PIECES):
        mix_far(p).wait_send()
    for k in range(1, count):
        dispatch(k).wait_send()
        giveback(k).wait_send()
    for g in range(GROUPS):
        rows_near(g).wait_send()
        rows_far(g).wait_send()
        rows_far_near(g).wait_send()
        part_near(0, g).wait_send()
        part_near(1, g).wait_send()
        part_far(g).wait_send()


def layer(
    glu_value,
    glu_gate,
    conv_kernel,
    norm_gain,
    mix_weight,
    residual,
    resid_gain,
    expert_ids,
    route_weight,
    w_gate,
    w_up,
    w_down,
    out_gain,
):
    count = lax.axis_size("sp")
    places = lax.axis_size("tp")
    length, channels = glu_value.shape
    block, width = residual.shape
    units = w_down.shape[1]
    top = expert_ids.shape[1]
    total = 2 * block * top
    size = total // GROUPS
    half = length // 2
    piece = width // PIECES
    low_type = glu_value.dtype
    anywhere = pl.BlockSpec(memory_space=pl.ANY)
    inside = pl.BlockSpec(memory_space=pltpu.VMEM)

    def vmem(*shape, dtype=low_type):
        return pltpu.VMEM(shape, dtype)

    def wide_vmem(*shape):
        return pltpu.VMEM(shape, jnp.float32)

    scratch = [
        vmem(length, channels),
        vmem(length, channels),
        vmem(channels, width),
        vmem(block, width),
        vmem(width, units),
        vmem(width, units),
        vmem(units, width),
        vmem(HALO, channels),
        vmem(HALO, channels),
        wide_vmem(length + HALO, channels),
        wide_vmem(2, half, channels),
        wide_vmem(2, 2, 8, 128),
        wide_vmem(2, places - 1, 2, 8, 128),
        vmem(2, half, channels),
        vmem(2, PIECES, half, piece),
        vmem(2, PIECES, block, piece),
        vmem(PIECES, block, piece),
        vmem(PIECES, block, piece),
        vmem(block, width),
        wide_vmem(count, block),
        wide_vmem(count, block),
        wide_vmem(total, block),
        wide_vmem(total, block),
        vmem(block, total),
        vmem(block, total),
        vmem(total, width),
        vmem(2, 2 * total, width),
        vmem(2, 2 * total, width),
        vmem(2, total, width),
        vmem(total, width),
        vmem(4 * size, units),
        vmem(total, width),
        wide_vmem(block, width),
        pltpu.SemaphoreType.DMA((7,)),
        pltpu.SemaphoreType.DMA,
        pltpu.SemaphoreType.DMA,
        pltpu.SemaphoreType.DMA((2, places - 1)),
        pltpu.SemaphoreType.DMA((2, places - 1)),
        pltpu.SemaphoreType.DMA((2, PIECES)),
        pltpu.SemaphoreType.DMA((2, PIECES)),
        pltpu.SemaphoreType.DMA((PIECES,)),
        pltpu.SemaphoreType.DMA((PIECES,)),
        pltpu.SemaphoreType.DMA((count,)),
        pltpu.SemaphoreType.DMA((count,)),
        pltpu.SemaphoreType.DMA((6, GROUPS)),
        pltpu.SemaphoreType.DMA((6, GROUPS)),
        pltpu.SemaphoreType.DMA((count,)),
        pltpu.SemaphoreType.DMA((count,)),
    ]
    return pl.pallas_call(
        functools.partial(layer_kernel, count, places),
        out_shape=jax.ShapeDtypeStruct((block, width), low_type),
        in_specs=[
            anywhere,
            anywhere,
            inside,
            inside,
            anywhere,
            anywhere,
            inside,
            inside,
            inside,
            anywhere,
            anywhere,
            anywhere,
            inside,
        ],
        out_specs=inside,
        scratch_shapes=scratch,
        compiler_params=pltpu.CompilerParams(
            collective_id=0, has_side_effects=True, vmem_limit_bytes=62 * 2**20
        ),
        cost_estimate=pl.CostEstimate(
            flops=24 * total * width * units,
            bytes_accessed=10 * total * width,
            transcendentals=4 * total * units,
        ),
        name="layer",
    )(
        glu_value,
        glu_gate,
        conv_kernel,
        norm_gain[None, :],
        mix_weight,
        residual,
        resid_gain[None, :],
        expert_ids.T,
        route_weight.T,
        w_gate[0],
        w_up[0],
        w_down[0],
        out_gain[None, :],
    )


def solution(mesh):
    in_specs = (
        P("sp", "tp"),
        P("sp", "tp"),
        P(None, "tp"),
        P("tp"),
        P("tp", None),
        P(("sp", "tp"), None),
        P(),
        P(("sp", "tp"), None),
        P(("sp", "tp"), None),
        P("sp", None, "tp"),
        P("sp", None, "tp"),
        P("sp", "tp", None),
        P(),
    )

    return jax.shard_map(
        layer,
        mesh=mesh,
        in_specs=in_specs,
        out_specs=P(("sp", "tp"), None),
        check_vma=False,
    )
```

```python
import functools

import jax
import jax.numpy as jnp
from jax import lax
from jax.experimental import pallas as pl
from jax.experimental.pallas import tpu as pltpu
from jax.sharding import PartitionSpec as P

EPSILON = 1e-05
LIMIT = 7.0
SLOPE = 1.702
HALO = 32
CHUNK = 64
PIECES = 4

MESH = pl.DeviceIdType.MESH
GROUPS = 8
ARRIVAL = (0, 1, 2, 4, 3, 5, 6, 7)


def flipped(index, mask):
    result = index
    bit = 1
    while bit <= mask:
        if mask & bit:
            result = result + bit - 2 * bit * lax.rem(lax.div(index, bit), 2)
        bit *= 2
    return result


def wide(values):
    return values.astype(jnp.float32)


def layer_kernel(
    count,
    places,
    value_hbm,
    glu_hbm,
    taps,
    norm_gain,
    mix_hbm,
    residual_hbm,
    resid_gain,
    ids,
    route,
    gate_hbm,
    up_hbm,
    down_hbm,
    out_gain,
    out,
    value,
    glu,
    mix,
    residual,
    gate,
    up,
    down,
    halo_out,
    halo_in,
    extended,
    convolved,
    stats,
    stats_in,
    mix_in,
    products,
    near_in,
    far_out,
    far_in,
    hidden,
    before,
    chosen,
    pick,
    weigh,
    high,
    low,
    slots,
    rows,
    outp,
    nrecv,
    frecv,
    act,
    returned,
    combined,
    load_sem,
    halo_send,
    halo_recv,
    stat_send,
    stat_recv,
    mixn_send,
    mixn_recv,
    mixf_send,
    mixf_recv,
    disp_send,
    disp_recv,
    hop_send,
    hop_recv,
    ret_send,
    ret_recv,
):
    me = lax.axis_index("sp")
    place = lax.axis_index("tp")
    near = flipped(place, 1)
    far = flipped(place, 2)
    across = flipped(place, 3)
    core = lax.rem(place, 2)
    side_x = lax.div(place, 2)

    length, channels = value.shape
    half = length // 2
    block = half // 2
    width = mix.shape[1]
    units = down.shape[0]
    total = slots.shape[0]
    cap = total // count
    size = total // GROUPS
    per = count // GROUPS
    piece = width // PIECES

    loads = [
        pltpu.make_async_copy(source, target, load_sem.at[i])
        for i, (source, target) in enumerate(
            (
                (value_hbm, value),
                (glu_hbm, glu),
                (mix_hbm, mix),
                (residual_hbm, residual),
                (gate_hbm, gate),
                (up_hbm, up),
                (down_hbm, down),
            )
        )
    ]
    for load in loads[:2]:
        load.start()

    following = lax.rem(me + 1, count)
    previous = lax.rem(me + count - 1, count)
    barrier = pltpu.get_barrier_semaphore()
    for k in range(1, count):
        pl.semaphore_signal(barrier, inc=1, device_id={"sp": flipped(me, k)}, device_id_type=MESH)
    for other in (near, far, across):
        pl.semaphore_signal(barrier, inc=1, device_id={"tp": other}, device_id_type=MESH)

    def gated(first, rows_at_once):
        span = pl.ds(first, rows_at_once)
        return (wide(value[span, :]) * jax.nn.sigmoid(wide(glu[span, :]))).astype(jnp.bfloat16)

    loads[0].wait()
    loads[1].wait()
    for load in loads[2:]:
        load.start()
    tail = gated(length - HALO, HALO)
    halo_out[...] = tail
    extended[pl.ds(length, HALO), :] = wide(tail)

    @pl.loop(0, length // CHUNK)
    def _(i):
        first = pl.multiple_of(i * CHUNK, CHUNK)
        extended[pl.ds(first + HALO, CHUNK), :] = wide(gated(first, CHUNK))

    pl.semaphore_wait(barrier, count + 2)
    halo = pltpu.make_async_remote_copy(
        src_ref=halo_out,
        dst_ref=halo_in,
        send_sem=halo_send,
        recv_sem=halo_recv,
        device_id={"sp": following},
        device_id_type=MESH,
    )

    @pl.when(me < count - 1)
    def _():
        halo.start()

    lanes = lax.broadcasted_iota(jnp.int32, (8, 128), 1)
    upper_first = (1, 0)
    turn = (1 - side_x, side_x)

    def convolve(h):
        def step(i, carry):
            sums, squares = carry
            first = pl.multiple_of(h * half + i * CHUNK, CHUNK)
            row_sum = jnp.zeros((CHUNK, 128), jnp.float32)
            row_square = jnp.zeros((CHUNK, 128), jnp.float32)
            for c in range(channels // 128):
                columns = pl.ds(c * 128, 128)
                window = extended[pl.ds(first, CHUNK + HALO), columns]
                result = jnp.zeros((CHUNK, 128), jnp.float32)
                reach = taps.shape[0]
                lead = HALO - reach + 1
                for phase in range(8):
                    moved = window
                    if phase:
                        moved = pltpu.roll(window, CHUNK + HALO - phase, 0)
                    for k in range(reach):
                        if (k + lead) % 8 == phase:
                            start = (k + lead) // 8 * 8
                            result = result + taps[k : k + 1, columns] * moved[start : start + CHUNK]
                convolved[h, pl.ds(pl.multiple_of(i * CHUNK, CHUNK), CHUNK), columns] = result
                row_sum = row_sum + result
                row_square = row_square + result * result
            for r in range(CHUNK // 8):
                here = lanes == i * (CHUNK // 8) + r
                part = jnp.sum(row_sum[8 * r : 8 * r + 8], axis=1, keepdims=True)
                sums = jnp.where(here, part, sums)
                part = jnp.sum(row_square[8 * r : 8 * r + 8], axis=1, keepdims=True)
                squares = jnp.where(here, part, squares)
            return sums, squares

        zero = jnp.zeros((8, 128), jnp.float32)
        sums, squares = lax.fori_loop(0, half // CHUNK, step, (zero, zero))
        stats[h, 0] = sums
        stats[h, 1] = squares

    def stat_copy(h, j, other):
        return pltpu.make_async_remote_copy(
            src_ref=stats.at[h],
            dst_ref=stats_in.at[h, j],
            send_sem=stat_send.at[h, j],
            recv_sem=stat_recv.at[h, j],
            device_id={"tp": other},
            device_id_type=MESH,
        )

    def stat_copies(h):
        return [stat_copy(h, j, other) for j, other in enumerate((near, far, across))]

    def normalized(order, owner):
        h = turn[order]
        both = stats[h] + stats_in[h, 0] + stats_in[h, 1] + stats_in[h, 2]
        centre = both[0] / (places * channels)
        scale = lax.rsqrt(both[1] / (places * channels) - centre * centre + EPSILON)

        @pl.loop(0, block // 16)
        def _(step):
            i = step + owner * (block // 16)
            parts = []
            for r in range(2):
                here = lanes == 2 * i + r
                middle = jnp.sum(jnp.where(here, centre, 0.0), axis=1, keepdims=True)
                factor = jnp.sum(jnp.where(here, scale, 0.0), axis=1, keepdims=True)
                first = pl.multiple_of(i * 16 + r * 8, 8)
                normed = (convolved[h, pl.ds(first, 8), :] - middle) * factor * norm_gain[...]
                parts.append(jax.nn.silu(normed))
            span = pl.ds(pl.multiple_of(i * 16, 16), 16)
            mix_in[order, span, :] = jnp.concatenate(parts, axis=0).astype(jnp.bfloat16)

    kept_rows = pl.ds(pl.multiple_of(core * block, block), block)
    given_rows = pl.ds(pl.multiple_of((1 - core) * block, block), block)

    def mix_near(h, p):
        return pltpu.make_async_remote_copy(
            src_ref=products.at[h, p, given_rows],
            dst_ref=near_in.at[h, p],
            send_sem=mixn_send.at[h, p],
            recv_sem=mixn_recv.at[h, p],
            device_id={"tp": near},
            device_id_type=MESH,
        )

    def mix_far(p):
        return pltpu.make_async_remote_copy(
            src_ref=far_out.at[p],
            dst_ref=far_in.at[p],
            send_sem=mixf_send.at[p],
            recv_sem=mixf_recv.at[p],
            device_id={"tp": far},
            device_id_type=MESH,
        )

    def project(order, span, p):
        products[order, p, span] = jnp.dot(
            mix_in[order, span, :],
            mix[:, p * piece : (p + 1) * piece],
            preferred_element_type=jnp.float32,
        ).astype(jnp.bfloat16)

    def project_half(order):
        for copy in stat_copies(turn[order]):
            copy.wait_recv()
        normalized(order, 1 - core)
        if order == 0:
            loads[2].wait()
        for p in range(PIECES):
            project(order, given_rows, p)
            if p:
                mix_near(order, p - 1).start()
        mix_near(order, PIECES - 1).start()
        normalized(order, core)
        for p in range(PIECES):
            project(order, kept_rows, p)
            if order == 0:
                mix_near(0, p).wait_recv()
                far_out[p] = (wide(products[0, p, kept_rows, :]) + wide(near_in[0, p])).astype(
                    jnp.bfloat16
                )
                mix_far(p).start()

    for h in upper_first:
        if h == 0:
            @pl.when(me > 0)
            def _():
                halo.wait_recv()
                extended[pl.ds(0, HALO), :] = wide(halo_in[...])

            @pl.when(me == 0)
            def _():
                extended[pl.ds(0, HALO), :] = jnp.zeros((HALO, channels), jnp.float32)
        convolve(h)
        for copy in stat_copies(h):
            copy.start()

    experts = lax.broadcasted_iota(jnp.int32, (count, block), 0)
    named = [ids[j : j + 1, :] == experts for j in range(ids.shape[0])]
    hits = jnp.zeros((count, block), jnp.float32)
    shares = jnp.zeros((count, block), jnp.float32)
    for j, match in enumerate(named):
        hits = hits + jnp.where(match, 1.0, 0.0)
        shares = shares + jnp.where(match, route[j : j + 1, :], 0.0)
    earlier = lax.broadcasted_iota(jnp.int32, (block, block), 0)
    later = lax.broadcasted_iota(jnp.int32, (block, block), 1)
    triangle = jnp.where(earlier < later, 1.0, 0.0).astype(jnp.bfloat16)
    ranks = jnp.dot(hits.astype(jnp.bfloat16), triangle, preferred_element_type=jnp.float32)
    before[...] = jnp.where(hits > 0.0, ranks, -1.0)
    chosen[...] = shares
    rank = lax.broadcasted_iota(jnp.int32, (cap, block), 0).astype(jnp.float32)
    for k in range(count):
        expert = flipped(me, k)
        match = before[pl.ds(expert, 1), :] == rank
        pick[pl.ds(k * cap, cap), :] = jnp.where(match, 1.0, 0.0)
        weigh[pl.ds(k * cap, cap), :] = jnp.where(match, chosen[pl.ds(expert, 1), :], 0.0)
    turned = weigh[...].T
    upper_part = turned.astype(jnp.bfloat16)
    high[...] = upper_part
    low[...] = (turned - wide(upper_part)).astype(jnp.bfloat16)

    project_half(0)
    project_half(1)

    def normalize(values, gain):
        centred = values - jnp.mean(values, axis=1, keepdims=True)
        spread = jnp.mean(centred * centred, axis=1, keepdims=True)
        return centred * lax.rsqrt(spread + EPSILON) * gain

    loads[3].wait()
    for p in range(PIECES):
        mix_near(1, p).wait_recv()
        columns = pl.ds(p * piece, piece)
        combined[:, columns] = (
            wide(residual[:, columns]) + wide(products[1, p, kept_rows, :]) + wide(near_in[1, p])
        )
    for p in range(PIECES):
        mix_far(p).wait_recv()

    @pl.loop(0, block // 32)
    def _(i):
        span = pl.ds(pl.multiple_of(i * 32, 32), 32)
        distant = jnp.concatenate([wide(far_in[p, span, :]) for p in range(PIECES)], axis=1)
        hidden[span, :] = normalize(combined[span, :] + distant, resid_gain[...]).astype(
            jnp.bfloat16
        )

    def spot(g, side):
        return pl.ds((2 * ARRIVAL.index(g) + side) * size, size)

    def spot_of(k):
        return pl.ds(2 * ARRIVAL.index(k // per) * size + (k % per) * cap, cap)

    def dispatched(k, first, extent, number):
        return pltpu.make_async_remote_copy(
            src_ref=slots.at[pl.ds(k * cap + first, extent)],
            dst_ref=rows.at[0, pl.ds(spot_of(k).start + first, extent)],
            send_sem=disp_send.at[number],
            recv_sem=disp_recv.at[number],
            device_id={"sp": flipped(me, k)},
            device_id_type=MESH,
        )

    def dispatch(k):
        if k == 1 and per == 1:
            return [dispatched(k, 0, cap // 2, 1), dispatched(k, cap // 2, cap // 2, 0)]
        return [dispatched(k, 0, cap, k)]

    def giveback(k):
        return pltpu.make_async_remote_copy(
            src_ref=outp.at[0, spot_of(k)],
            dst_ref=returned.at[pl.ds(k * cap, cap)],
            send_sem=ret_send.at[k],
            recv_sem=ret_recv.at[k],
            device_id={"sp": flipped(me, k)},
            device_id_type=MESH,
        )

    def hop(kind, g, source, target, other):
        return pltpu.make_async_remote_copy(
            src_ref=source,
            dst_ref=target,
            send_sem=hop_send.at[kind, g],
            recv_sem=hop_recv.at[kind, g],
            device_id={"tp": other},
            device_id_type=MESH,
        )

    def rows_near(g):
        return hop(0, g, rows.at[0, spot(g, 0)], rows.at[0, spot(g, 1)], near)

    def rows_far(g):
        return hop(1, g, rows.at[0, spot(g, 0)], rows.at[1, spot(g, 0)], far)

    def rows_far_part(i):
        span = pl.ds(spot(1, 0).start + i * (size // 2), size // 2)
        return hop(6 * i + 1 - i, 1, rows.at[0, span], rows.at[1, span], far)

    def rows_far_all(g):
        return [rows_far_part(0), rows_far_part(1)] if g == 1 else [rows_far(g)]

    def rows_far_near(g):
        return hop(2, g, rows.at[1, spot(g, 0)], rows.at[1, spot(g, 1)], near)

    def part_near(side, g):
        return hop(
            3 + side, g, outp.at[side, spot(g, 1)], nrecv.at[side, pl.ds(g * size, size)], near
        )

    def part_far(g):
        return hop(5, g, outp.at[1, spot(g, 0)], frecv.at[pl.ds(g * size, size)], far)

    def forward(g):
        copies = [copy for k in range(g * per, (g + 1) * per) if k for copy in dispatch(k)]
        sends = rows_far_all(g)
        share = -(-len(copies) // len(sends))
        for i, send in enumerate(sends):
            for copy in copies[i * share : (i + 1) * share]:
                copy.wait_recv()
            send.start()
        rows_near(g).start()

    def send_group(g):
        for k in range(g * per, (g + 1) * per):
            if k:
                for copy in dispatch(k):
                    copy.start()
        if g == 0 and per == 1:
            forward(g)

    for index, g in enumerate(ARRIVAL):
        span = pl.ds(g * size, size)
        picked = jnp.dot(
            pick[span, :].astype(jnp.bfloat16), hidden[...], preferred_element_type=jnp.float32
        ).astype(jnp.bfloat16)
        slots[span, :] = picked
        if g == 0:
            rows[0, spot_of(0), :] = slots[pl.ds(0, cap), :]
        if index:
            send_group(ARRIVAL[index - 1])
    send_group(ARRIVAL[-1])
    if per > 1:
        forward(0)

    def forward_far(g):
        for copy in rows_far_all(g):
            copy.wait_recv()
        rows_far_near(g).start()

    def compute(side, *both):
        for g in both:
            (rows_far_near(g) if side else rows_near(g)).wait_recv()
        if side == 0 and 0 in both:
            loads[4].wait()
            loads[5].wait()
        count_rows = 2 * size * len(both)
        tile = pl.ds(2 * ARRIVAL.index(both[0]) * size, count_rows)
        step = min(256, units)

        @pl.loop(0, units // step)
        def _(j):
            columns = pl.ds(pl.multiple_of(j * step, step), step)
            tokens = rows[side, tile, :]
            gate_pre = jnp.dot(tokens, gate[:, columns], preferred_element_type=jnp.float32)
            up_pre = jnp.dot(tokens, up[:, columns], preferred_element_type=jnp.float32)
            clipped = jnp.minimum(gate_pre, LIMIT)
            upper = jnp.clip(up_pre, -LIMIT, LIMIT)
            act[:count_rows, columns] = (
                (upper + 1.0) * clipped * jax.nn.sigmoid(SLOPE * clipped)
            ).astype(jnp.bfloat16)

        if side == 0 and 0 in both:
            loads[6].wait()

        @pl.loop(0, PIECES)
        def _(j):
            columns = pl.ds(pl.multiple_of(j * piece, piece), piece)
            outp[side, tile, columns] = jnp.dot(
                act[:count_rows, :], down[:, columns], preferred_element_type=jnp.float32
            ).astype(jnp.bfloat16)

        for g in both:
            part_near(side, g).start()

    def chip_sum(g):
        part_near(1, g).wait_recv()
        mine = wide(outp[1, spot(g, 0), :])
        other = wide(nrecv[1, pl.ds(g * size, size), :])
        outp[1, spot(g, 0), :] = (mine + other).astype(jnp.bfloat16)
        part_far(g).start()

    def finish(g):
        part_near(0, g).wait_recv()
        mine = wide(outp[0, spot(g, 0), :])
        other = wide(nrecv[0, pl.ds(g * size, size), :])
        part_far(g).wait_recv()
        distant = wide(frecv[pl.ds(g * size, size), :])
        outp[0, spot(g, 0), :] = (mine + other + distant).astype(jnp.bfloat16)
        for k in range(g * per, (g + 1) * per):
            if k:
                giveback(k).start()
            else:
                returned[pl.ds(0, cap), :] = outp[0, spot_of(0), :]

    def combine(pair):
        for k in range(2 * pair * per, 2 * (pair + 1) * per):
            if k:
                giveback(k).wait_recv()
        inner = slice(2 * pair * size, 2 * (pair + 1) * size)
        for p in range(PIECES):
            columns = slice(p * piece, (p + 1) * piece)
            values = returned[inner, columns]
            combined[:, columns] += jnp.dot(
                high[:, inner], values, preferred_element_type=jnp.float32
            ) + jnp.dot(low[:, inner], values, preferred_element_type=jnp.float32)

    forward(1)
    forward_far(0)
    compute(0, 0, 1)
    forward(2)
    forward(4)
    forward_far(1)
    compute(1, 0, 1)
    compute(0, 2, 4)
    forward(3)
    forward_far(2)
    forward_far(4)
    compute(1, 2, 4)
    forward(5)
    chip_sum(4)
    compute(0, 3, 5)
    forward_far(3)
    forward(6)
    forward_far(5)
    compute(1, 3, 5)
    forward(7)
    finish(4)
    chip_sum(5)
    chip_sum(1)
    forward_far(6)
    compute(1, 6)
    finish(5)
    chip_sum(6)
    forward_far(7)
    compute(1, 7)
    chip_sum(7)
    compute(0, 6, 7)
    chip_sum(2)
    chip_sum(3)
    chip_sum(0)
    combined[...] = wide(hidden[...])
    finish(1)
    finish(6)
    finish(7)
    finish(2)
    combine(2)
    finish(3)
    finish(0)
    combine(1)
    combine(0)
    combine(3)

    @pl.loop(0, block // 32)
    def _(i):
        span = pl.ds(pl.multiple_of(i * 32, 32), 32)
        out[span, :] = normalize(combined[span, :], out_gain[...]).astype(jnp.bfloat16)

    @pl.when(me < count - 1)
    def _():
        halo.wait_send()

    for h in range(2):
        for copy in stat_copies(h):
            copy.wait_send()
        for p in range(PIECES):
            mix_near(h, p).wait_send()
    for p in range(PIECES):
        mix_far(p).wait_send()
    for k in range(1, count):
        for copy in dispatch(k):
            copy.wait_send()
        giveback(k).wait_send()
    for g in range(GROUPS):
        rows_near(g).wait_send()
        for copy in rows_far_all(g):
            copy.wait_send()
        rows_far_near(g).wait_send()
        part_near(0, g).wait_send()
        part_near(1, g).wait_send()
        part_far(g).wait_send()


def layer(
    glu_value,
    glu_gate,
    conv_kernel,
    norm_gain,
    mix_weight,
    residual,
    resid_gain,
    expert_ids,
    route_weight,
    w_gate,
    w_up,
    w_down,
    out_gain,
):
    count = lax.axis_size("sp")
    places = lax.axis_size("tp")
    length, channels = glu_value.shape
    block, width = residual.shape
    units = w_down.shape[1]
    top = expert_ids.shape[1]
    total = 2 * block * top
    size = total // GROUPS
    half = length // 2
    piece = width // PIECES
    low_type = glu_value.dtype
    anywhere = pl.BlockSpec(memory_space=pl.ANY)
    inside = pl.BlockSpec(memory_space=pltpu.VMEM)

    def vmem(*shape, dtype=low_type):
        return pltpu.VMEM(shape, dtype)

    def wide_vmem(*shape):
        return pltpu.VMEM(shape, jnp.float32)

    scratch = [
        vmem(length, channels),
        vmem(length, channels),
        vmem(channels, width),
        vmem(block, width),
        vmem(width, units),
        vmem(width, units),
        vmem(units, width),
        vmem(HALO, channels),
        vmem(HALO, channels),
        wide_vmem(length + HALO, channels),
        wide_vmem(2, half, channels),
        wide_vmem(2, 2, 8, 128),
        wide_vmem(2, places - 1, 2, 8, 128),
        vmem(2, half, channels),
        vmem(2, PIECES, half, piece),
        vmem(2, PIECES, block, piece),
        vmem(PIECES, block, piece),
        vmem(PIECES, block, piece),
        vmem(block, width),
        wide_vmem(count, block),
        wide_vmem(count, block),
        wide_vmem(total, block),
        wide_vmem(total, block),
        vmem(block, total),
        vmem(block, total),
        vmem(total, width),
        vmem(2, 2 * total, width),
        vmem(2, 2 * total, width),
        vmem(2, total, width),
        vmem(total, width),
        vmem(4 * size, units),
        vmem(total, width),
        wide_vmem(block, width),
        pltpu.SemaphoreType.DMA((7,)),
        pltpu.SemaphoreType.DMA,
        pltpu.SemaphoreType.DMA,
        pltpu.SemaphoreType.DMA((2, places - 1)),
        pltpu.SemaphoreType.DMA((2, places - 1)),
        pltpu.SemaphoreType.DMA((2, PIECES)),
        pltpu.SemaphoreType.DMA((2, PIECES)),
        pltpu.SemaphoreType.DMA((PIECES,)),
        pltpu.SemaphoreType.DMA((PIECES,)),
        pltpu.SemaphoreType.DMA((count,)),
        pltpu.SemaphoreType.DMA((count,)),
        pltpu.SemaphoreType.DMA((7, GROUPS)),
        pltpu.SemaphoreType.DMA((7, GROUPS)),
        pltpu.SemaphoreType.DMA((count,)),
        pltpu.SemaphoreType.DMA((count,)),
    ]
    return pl.pallas_call(
        functools.partial(layer_kernel, count, places),
        out_shape=jax.ShapeDtypeStruct((block, width), low_type),
        in_specs=[
            anywhere,
            anywhere,
            inside,
            inside,
            anywhere,
            anywhere,
            inside,
            inside,
            inside,
            anywhere,
            anywhere,
            anywhere,
            inside,
        ],
        out_specs=inside,
        scratch_shapes=scratch,
        compiler_params=pltpu.CompilerParams(
            collective_id=0, has_side_effects=True, vmem_limit_bytes=62 * 2**20
        ),
        cost_estimate=pl.CostEstimate(
            flops=24 * total * width * units,
            bytes_accessed=10 * total * width,
            transcendentals=4 * total * units,
        ),
        name="layer",
    )(
        glu_value,
        glu_gate,
        conv_kernel,
        norm_gain[None, :],
        mix_weight,
        residual,
        resid_gain[None, :],
        expert_ids.T,
        route_weight.T,
        w_gate[0],
        w_up[0],
        w_down[0],
        out_gain[None, :],
    )


def solution(mesh):
    in_specs = (
        P("sp", "tp"),
        P("sp", "tp"),
        P(None, "tp"),
        P("tp"),
        P("tp", None),
        P(("sp", "tp"), None),
        P(),
        P(("sp", "tp"), None),
        P(("sp", "tp"), None),
        P("sp", None, "tp"),
        P("sp", None, "tp"),
        P("sp", "tp", None),
        P(),
    )

    return jax.shard_map(
        layer,
        mesh=mesh,
        in_specs=in_specs,
        out_specs=P(("sp", "tp"), None),
        check_vma=False,
    )
```
